32 devices in a mesh: sp: 8 (over z, y), tp: 4 (over x, core).
Axes of the slice: x: 2, y: 2, z: 4, core: 2. Of those that a mesh axis runs over, the one named last changes fastest.
Arguments:
- queries: bfloat16 [8192, 1024], P('sp', 'tp'), may hold values from -6 to 6
- cell_key_rows: bfloat16 [8192, 1024], P('sp', 'tp'), may hold values from -6 to 6
- cell_value_rows: bfloat16 [8192, 2048], P('sp', 'tp'), may hold values from -6 to 6
- output_gate_logits: bfloat16 [8192, 2048], P('sp', 'tp'), may hold values from -6 to 6
- input_gate_logits: bfloat16 [8, 8192], P('tp', 'sp'), may hold values from -4 to 216
- forget_gate_logits: bfloat16 [8, 8192], P('tp', 'sp'), may hold values from 0.5 to 14
- forget_extra_term: float32 [8, 8192], P('tp', 'sp'), may hold values from -1.4 to 0
- residual: bfloat16 [8192, 2048], P('sp', 'tp'), may hold values from -13 to 13
- head_norm_gain: bfloat16 [2048], P('tp'), may hold values from 0.099609375 to 1.8984375
- cell_output_weight: bfloat16 [2048, 2048], P('tp'), may hold values from -0.25 to 0.25
- feedforward_norm_gain: bfloat16 [2048], replicated, may hold values from 0.099609375 to 1.8984375
- gate_projection_weight: bfloat16 [2048, 5632], P('sp', 'tp'), may hold values from -0.125 to 0.125
- up_projection_weight: bfloat16 [2048, 5632], P('sp', 'tp'), may hold values from -0.125 to 0.125
- down_projection_weight: bfloat16 [5632, 2048], P('tp', 'sp'), may hold values from -0.15625 to 0.15625
Outputs:
- mixed: bfloat16 [8192, 2048], P('sp', 'tp')
The draws below stay inside these ranges and needn't reach their ends.
All inputs are finite; a program needn't handle non-finite values.
Results may differ from the reference program's by a relative error of at most 0.017.
Values may be sent and summed in bfloat16 or wider, within the bound.
A program may use at most 128 MiB of HBM per device.

```python
import jax
import jax.numpy as jnp
from jax import lax

D = 2048
HEADS = 8
DK = 128
DV = 256
FF = 5632
TOK_DEV = 1024
TOKENS = 8192
N_TP = 4


def draw_input_gate_logits(key, part):
    base_key = jax.random.fold_in(key, 11)
    values = jnp.clip(jax.random.normal(base_key, (HEADS, TOKENS), jnp.float32), -4.0, 4.0)
    return values.astype(jnp.bfloat16)


def draw_forget_gate_logits(key, part):
    order = jax.random.permutation(jax.random.fold_in(key, 21), HEADS)
    noise_key = jax.random.fold_in(key, 22)
    slow_count = HEADS // 2
    jitter = 0.6 * jnp.clip(jax.random.normal(noise_key, (HEADS, TOKENS), jnp.float32), -4.0, 4.0)
    slow_heads = order < slow_count
    quick = jnp.log(jax.random.uniform(jax.random.fold_in(key, 23), (HEADS,), jnp.float32, 30.0, 60.0))
    level = jnp.where(slow_heads, jnp.log(TOKENS / 0.8), quick)
    block_shift = jax.random.uniform(jax.random.fold_in(key, 24), (HEADS, TOKENS // TOK_DEV), jnp.float32, -0.4, 0.4)
    shifts = jnp.repeat(block_shift, TOK_DEV, axis=1)
    return (level[:, None] + shifts + jitter).astype(jnp.bfloat16)


def draw_forget_extra_term(key, part):
    spots = jax.random.randint(jax.random.fold_in(key, 31), (HEADS, 2, 1), 0, TOKENS)
    fraction = jax.random.uniform(jax.random.fold_in(key, 32), (HEADS, 2, 1), jnp.float32, 0.2, 0.5)
    depth = jnp.log(1.0 - fraction)
    places = jnp.arange(TOKENS)[None, None, :]
    return jnp.sum(jnp.where(places == spots, depth, 0.0), axis=1).astype(jnp.float32)


def draw_residual(key, part):
    column_scale = 0.4 * 6.0 ** (jnp.arange(D, dtype=jnp.float32) / D)
    values = jnp.clip(jax.random.normal(jax.random.fold_in(key, 41), (TOKENS, D), jnp.float32), -4.0, 4.0)
    return (values * column_scale[None, :]).astype(jnp.bfloat16)


def block_levels(rng, dims, shards, low, largest):
    factor_of, own = 1.0, jax.random.fold_in(rng, 6)
    for position, parts in shards:
        steps = jnp.exp(jax.random.uniform(jax.random.fold_in(own, position), (parts,), jnp.float32, low / len(shards), largest / len(shards)))
        factor_of = factor_of * jnp.repeat(steps, dims[position] // parts).reshape([-1 if axis == position else 1 for axis in range(len(dims))])
    return factor_of


def normal_values(rng, shape, spread, most, split=(), held_as=jnp.bfloat16):
    loudness = block_levels(rng, shape, split, -0.22, 0.18) if split else 1.0
    result = jax.random.normal(rng, shape, jnp.float32) * spread * loudness
    return jnp.minimum(jnp.maximum(result, -most), most).astype(held_as)


def setup_inputs(seed: int = 0) -> dict:
    arg_keys = jax.random.split(jax.random.key(seed), 15)
    return {
        "queries": normal_values(arg_keys[0], (TOKENS, HEADS * DK), 1.0, 6.0, ((0, 8), (1, 4))),
        "cell_key_rows": normal_values(arg_keys[1], (TOKENS, HEADS * DK), 1.0, 6.0, ((0, 8), (1, 4))),
        "cell_value_rows": normal_values(arg_keys[2], (TOKENS, HEADS * DV), 1.0, 6.0, ((0, 8), (1, 4))),
        "output_gate_logits": normal_values(arg_keys[3], (TOKENS, HEADS * DV), 1.0, 6.0, ((0, 8), (1, 4))),
        "input_gate_logits": draw_input_gate_logits(jax.random.fold_in(arg_keys[14], 71), 0),
        "forget_gate_logits": draw_forget_gate_logits(jax.random.fold_in(arg_keys[14], 71), 0),
        "forget_extra_term": draw_forget_extra_term(jax.random.fold_in(arg_keys[14], 71), 0),
        "residual": draw_residual(jax.random.fold_in(arg_keys[14], 71), 0),
        "head_norm_gain": jnp.clip(1.0 + 0.18 * jax.random.normal(arg_keys[8], (HEADS * DV,), jnp.float32), 0.099609375, 1.8984375).astype(jnp.bfloat16),
        "cell_output_weight": normal_values(arg_keys[9], (HEADS * DV, D), (HEADS * DV // 4) ** -0.5, 0.25, ((0, 4),)),
        "feedforward_norm_gain": jnp.clip(1.0 + 0.18 * jax.random.normal(arg_keys[10], (D,), jnp.float32), 0.099609375, 1.8984375).astype(jnp.bfloat16),
        "gate_projection_weight": normal_values(arg_keys[11], (D, FF), D ** -0.5, 0.125, ((0, 8), (1, 4))),
        "up_projection_weight": normal_values(arg_keys[12], (D, FF), D ** -0.5, 0.125, ((0, 8), (1, 4))),
        "down_projection_weight": normal_values(arg_keys[13], (FF, D), (FF // 4) ** -0.5, 0.15625, ((0, 4), (1, 8))),
    }


PRECISE = lax.Precision.HIGHEST
LOWEST_LOG = -1e+30
EPSILON = 1e-06

def to_blocks(array, block_count, block_size):
    shaped = array.reshape((array.shape[0], block_count, block_size) + array.shape[2:])
    return jnp.moveaxis(shaped, 1, 0)

def from_blocks(array):
    moved = jnp.moveaxis(array, 0, 1)
    return moved.reshape((moved.shape[0], moved.shape[1] * moved.shape[2]) + moved.shape[3:])

def memory_blocks(query_heads, key_heads, value_heads, in_gates, forget_log_value, block_size):
    head_count, length, key_width = query_heads.shape
    value_width = value_heads.shape[2]
    block_count = length // block_size
    causal = jnp.tril(jnp.ones((block_size, block_size), bool))

    def advance(carried, pieces):
        memory_state, top_log, offset = carried
        query_block, key_block, value_block, gate_block, forget_block = pieces
        running = jnp.cumsum(forget_block, axis=-1)
        log_weight = jnp.where(causal, running[:, :, None] - running[:, None, :] + gate_block[:, None, :], -jnp.inf)
        log_start = running + top_log[:, None]
        row_max = jnp.maximum(lax.optimization_barrier(jnp.max(log_weight, axis=-1)), log_start)
        scores = jnp.einsum('htd,hsd->hts', query_block, key_block, precision=PRECISE)
        scores = scores * jnp.exp(log_weight - row_max[:, :, None])
        earlier = jnp.einsum('htd,hde->hte', query_block, memory_state, precision=PRECISE)
        numerator = jnp.exp(log_start - row_max)[:, :, None] * earlier
        numerator = numerator + jnp.einsum('hts,hse->hte', scores, value_block, precision=PRECISE)
        last_cum = running[:, -1]
        log_end = last_cum[:, None] - running + gate_block
        new_top = jnp.maximum(last_cum + top_log, lax.optimization_barrier(jnp.max(log_end, axis=-1)))
        scaled = key_block * jnp.exp(log_end - new_top[:, None])[:, :, None]
        memory_state = jnp.exp(last_cum + top_log - new_top)[:, None, None] * memory_state
        memory_state = memory_state + jnp.einsum('hsd,hse->hde', scaled, value_block, precision=PRECISE)
        return ((memory_state, new_top, offset + last_cum), (numerator, row_max, offset[:, None] + running))
    initial = (jnp.zeros((head_count, key_width, value_width), jnp.float32), jnp.full((head_count,), LOWEST_LOG, jnp.float32), jnp.zeros((head_count,), jnp.float32))
    pieces = tuple((to_blocks(array, block_count, block_size) for array in (query_heads, key_heads, value_heads, in_gates, forget_log_value)))
    ending, outputs = lax.scan(advance, initial, pieces)
    return (tuple((from_blocks(output) for output in outputs)), ending)

def reference(queries, cell_key_rows, cell_value_rows, output_gate_logits, input_gate_logits, forget_gate_logits, forget_extra_term, residual, head_norm_gain, cell_output_weight, feedforward_norm_gain, gate_projection_weight, up_projection_weight, down_projection_weight):
    length = queries.shape[0]

    def heads_first(array, width):
        return jnp.transpose(array.reshape(length, HEADS, width), (1, 0, 2)).astype(jnp.float32)
    query_heads = heads_first(queries, DK) * DK ** (-0.5)
    key_heads = heads_first(cell_key_rows, DK)
    value_heads = heads_first(cell_value_rows, DV)
    forget_log_value = jax.nn.log_sigmoid(forget_gate_logits.astype(jnp.float32)) + forget_extra_term
    results, _ = memory_blocks(query_heads, key_heads, value_heads, input_gate_logits.astype(jnp.float32), forget_log_value, min(length, 256))
    memory = jnp.transpose(results[0], (1, 0, 2))
    normal = memory * lax.rsqrt(lax.optimization_barrier(jnp.mean(memory * memory, axis=-1, keepdims=True)) + EPSILON)
    gate_open = jax.nn.sigmoid(output_gate_logits.astype(jnp.float32).reshape(length, HEADS, DV))
    gated_heads = normal * head_norm_gain.astype(jnp.float32).reshape(HEADS, DV) * gate_open
    gated_heads = gated_heads.reshape(length, HEADS * DV).astype(jnp.bfloat16)
    head_width = HEADS * DV // N_TP
    stream_sum = residual.astype(jnp.float32)
    for head_part in range(N_TP):
        head_lower = head_part * head_width
        head_term = jnp.dot(gated_heads[:, head_lower:head_lower + head_width], cell_output_weight[head_lower:head_lower + head_width], preferred_element_type=jnp.float32)
        head_rounded = lax.optimization_barrier(head_term.astype(jnp.bfloat16))
        stream_sum = stream_sum + head_rounded.astype(jnp.float32)
    stream = stream_sum.astype(jnp.bfloat16)
    stream_wide = stream.astype(jnp.float32)
    scale = lax.rsqrt(lax.optimization_barrier(jnp.mean(stream_wide * stream_wide, axis=-1, keepdims=True)) + EPSILON)
    normed = (stream_wide * scale * feedforward_norm_gain.astype(jnp.float32)).astype(jnp.bfloat16)
    gate_value = jnp.dot(normed, gate_projection_weight, preferred_element_type=jnp.float32)
    lifted = jnp.dot(normed, up_projection_weight, preferred_element_type=jnp.float32)
    hidden = (jax.nn.silu(gate_value) * lifted).astype(jnp.bfloat16)
    part_width = FF // N_TP
    summed = jnp.zeros(stream_wide.shape, jnp.float32)
    for part_index in range(N_TP):
        lower = part_index * part_width
        partial_value = jnp.dot(hidden[:, lower:lower + part_width], down_projection_weight[lower:lower + part_width], preferred_element_type=jnp.float32)
        rounded = lax.optimization_barrier(partial_value.astype(jnp.bfloat16))
        summed = summed + rounded.astype(jnp.float32)
    return (stream_wide + 0.5 * summed).astype(jnp.bfloat16)
```

```python
import jax
import jax.numpy as jnp
from jax import lax
from jax.experimental import pallas as pl
from jax.experimental.pallas import tpu as pltpu
from jax.sharding import PartitionSpec as P

LOWEST_LOG = -1e30
EPSILON = 1e-06


def shift_pairs(length, step):
    return [(source, source + step) for source in range(length - step)]


def entering_state(state, top, total):
    length, index = lax.axis_size("sp"), lax.axis_index("sp")
    heads, key_width, value_width = state.shape

    def pack(s, t, f):
        tail = jnp.zeros((heads, 8, value_width), jnp.float32)
        tail = tail.at[:, 0, :].set(t[:, None]).at[:, 1, :].set(f[:, None])
        return jnp.concatenate([s, tail], axis=1)

    def unpack(p, valid):
        s = p[:, :key_width, :]
        t = jnp.where(valid, p[:, key_width, 0], LOWEST_LOG)
        f = jnp.where(valid, p[:, key_width + 1, 0], 0.0)
        return jnp.where(valid, s, 0.0), t, f

    moved = lax.ppermute(pack(state, top, total), "sp", shift_pairs(length, 1))
    s, t, f = unpack(moved, index >= 1)
    step = 1
    while step < length - 1:
        moved = lax.ppermute(pack(s, t, f), "sp", shift_pairs(length, step))
        s0, t0, f0 = unpack(moved, index >= step)
        from_top = t0 + f
        new_top = jnp.maximum(from_top, t)
        s = (
            jnp.exp(from_top - new_top)[:, None, None] * s0
            + jnp.exp(t - new_top)[:, None, None] * s
        )
        t, f = new_top, f0 + f
        step *= 2
    return s, t


def cell_kernel(q_ref, k_ref, v_ref, a_ref, m_ref, c_ref, state_ref, open_ref, gain_ref, o_ref, *, scale):
    block = q_ref.shape[0]
    length = k_ref.shape[0]
    q = q_ref[...]
    first = pl.program_id(1) * block
    scores = lax.dot_general(
        q, k_ref[...], (((1,), (1,)), ((), ())), preferred_element_type=jnp.float32
    )
    rows = first + lax.broadcasted_iota(jnp.int32, (block, length), 0)
    cols = lax.broadcasted_iota(jnp.int32, (block, length), 1)
    weight = jnp.where(cols <= rows, jnp.exp(jnp.minimum(a_ref[0] - m_ref[0], 0.0)), 0.0)
    numer = jnp.dot(
        (scores * weight).astype(jnp.bfloat16), v_ref[...], preferred_element_type=jnp.float32
    )
    before = jnp.dot(q, state_ref[0].astype(jnp.bfloat16), preferred_element_type=jnp.float32)
    memory = (numer + c_ref[0] * before) * scale
    normal = memory * lax.rsqrt(jnp.mean(memory * memory, axis=-1, keepdims=True) + EPSILON)
    gate_open = jax.nn.sigmoid(open_ref[...].astype(jnp.float32))
    o_ref[...] = (normal * gain_ref[...].astype(jnp.float32) * gate_open).astype(o_ref.dtype)


def cell(queries, keys, values, a_log, m_col, c_col, state, open_logits, gain):
    heads, length = a_log.shape
    dk, dv = queries.shape[1] // heads, values.shape[1] // heads
    block = min(length, 256)
    return pl.pallas_call(
        lambda *refs: cell_kernel(*refs, scale=dk ** (-0.5)),
        grid=(heads, length // block),
        in_specs=[
            pl.BlockSpec((block, dk), lambda h, i: (i, h)),
            pl.BlockSpec((length, dk), lambda h, i: (0, h)),
            pl.BlockSpec((length, dv), lambda h, i: (0, h)),
            pl.BlockSpec((1, 1, length), lambda h, i: (h, 0, 0)),
            pl.BlockSpec((1, block, 1), lambda h, i: (h, i, 0)),
            pl.BlockSpec((1, block, 1), lambda h, i: (h, i, 0)),
            pl.BlockSpec((1, dk, dv), lambda h, i: (h, 0, 0)),
            pl.BlockSpec((block, dv), lambda h, i: (i, h)),
            pl.BlockSpec((1, dv), lambda h, i: (0, h)),
        ],
        out_specs=pl.BlockSpec((block, dv), lambda h, i: (i, h)),
        out_shape=jax.ShapeDtypeStruct((length, heads * dv), jnp.bfloat16),
        cost_estimate=pl.CostEstimate(
            flops=8 * heads * length * length * dv, bytes_accessed=6 * length * heads * dv, transcendentals=0
        ),
        name="cell",
    )(queries, keys, values, a_log[:, None, :], m_col[:, :, None], c_col[:, :, None], state, open_logits, gain)


def partner_pairs(count):
    return [(i, i ^ 1) for i in range(count)]


def ring_pairs(count, step):
    return [(i, (i + 2 * step) % count) for i in range(count)]


def take(array, index):
    return lax.dynamic_index_in_dim(array, index, 1, keepdims=False)


def product_scattered(rows, weight):
    count, index = lax.axis_size("tp"), lax.axis_index("tp")
    chips, core, chip = count // 2, index % 2, index // 2
    width = weight.shape[1] // count
    split = weight.reshape(weight.shape[0], chips, 2, width)

    def half(which):
        chosen = lax.dynamic_index_in_dim(split, which, 2, keepdims=False)
        return jnp.dot(
            rows, chosen.reshape(weight.shape[0], chips * width), preferred_element_type=jnp.float32
        )

    given = half(1 - core).astype(jnp.bfloat16)
    got = lax.ppermute(given, "tp", partner_pairs(count))
    kept = half(core).astype(jnp.bfloat16)
    shape = (rows.shape[0], chips, width)
    kept, got = kept.reshape(shape), got.reshape(shape)
    total = take(kept, chip).astype(jnp.float32) + take(got, chip).astype(jnp.float32)
    for step in range(1, chips):
        to = (chip + step) % chips
        sent = take(kept, to).astype(jnp.float32) + take(got, to).astype(jnp.float32)
        total = total + lax.ppermute(
            sent.astype(jnp.bfloat16), "tp", ring_pairs(count, step)
        ).astype(jnp.float32)
    return total


def columns_gathered(block):
    count, index = lax.axis_size("tp"), lax.axis_index("tp")
    chips, core, chip = count // 2, index % 2, index // 2
    width = block.shape[1]
    whole = jnp.zeros((block.shape[0], count * width), block.dtype)
    held = [(chip, block)]
    for step in range(1, chips):
        moved = lax.ppermute(block, "tp", ring_pairs(count, step))
        held.append(((chip - step) % chips, moved))
    for place, piece in held:
        other = lax.ppermute(piece, "tp", partner_pairs(count))
        whole = lax.dynamic_update_slice(whole, piece, (0, (2 * place + core) * width))
        whole = lax.dynamic_update_slice(whole, other, (0, (2 * place + 1 - core) * width))
    return whole


def local(
    queries,
    cell_key_rows,
    cell_value_rows,
    output_gate_logits,
    input_gate_logits,
    forget_gate_logits,
    forget_extra_term,
    residual,
    head_norm_gain,
    cell_output_weight,
    feedforward_norm_gain,
    gate_projection_weight,
    up_projection_weight,
    down_projection_weight,
):
    whole_gate = lax.all_gather(gate_projection_weight, "sp", axis=0, tiled=True)
    whole_up = lax.all_gather(up_projection_weight, "sp", axis=0, tiled=True)
    whole_down = lax.all_gather(down_projection_weight, "sp", axis=1, tiled=True)
    length = queries.shape[0]
    heads = input_gate_logits.shape[0]
    dk, dv = queries.shape[1] // heads, cell_value_rows.shape[1] // heads
    log_forget = jax.nn.log_sigmoid(forget_gate_logits.astype(jnp.float32)) + forget_extra_term
    running = jnp.cumsum(log_forget, axis=-1)
    a_log = input_gate_logits.astype(jnp.float32) - running
    m_log = lax.cummax(a_log, axis=1)
    a_top, total = m_log[:, -1], running[:, -1]
    decay = jnp.exp(a_log - a_top[:, None])
    weighed = (
        cell_key_rows.reshape(length, heads, dk).astype(jnp.float32) * decay.T[:, :, None]
    ).astype(jnp.bfloat16)
    state = jnp.stack(
        [
            lax.dot_general(
                weighed[:, h],
                cell_value_rows[:, h * dv : (h + 1) * dv],
                (((0,), (0,)), ((), ())),
                preferred_element_type=jnp.float32,
            )
            for h in range(heads)
        ]
    )
    carried, carried_top = entering_state(state, a_top + total, total)
    m_all = jnp.maximum(m_log, carried_top[:, None])
    coefficient = jnp.exp(carried_top[:, None] - m_all)
    gated = cell(
        queries,
        cell_key_rows,
        cell_value_rows,
        a_log,
        m_all,
        coefficient,
        carried,
        output_gate_logits,
        head_norm_gain[None, :],
    )
    summed = product_scattered(gated, cell_output_weight)
    stream = (residual.astype(jnp.float32) + summed).astype(jnp.bfloat16)
    wide = columns_gathered(stream).astype(jnp.float32)
    scale = lax.rsqrt(jnp.mean(wide * wide, axis=-1, keepdims=True) + EPSILON)
    normed = (wide * scale * feedforward_norm_gain.astype(jnp.float32)[None, :]).astype(jnp.bfloat16)
    gate_value = jnp.dot(normed, whole_gate, preferred_element_type=jnp.float32)
    lifted = jnp.dot(normed, whole_up, preferred_element_type=jnp.float32)
    hidden = (jax.nn.silu(gate_value) * lifted).astype(jnp.bfloat16)
    channel_total = product_scattered(hidden, whole_down)
    return (stream.astype(jnp.float32) + 0.5 * channel_total).astype(jnp.bfloat16)


def solution(mesh):
    placed = (
        P("sp", "tp"),
        P("sp", "tp"),
        P("sp", "tp"),
        P("sp", "tp"),
        P("tp", "sp"),
        P("tp", "sp"),
        P("tp", "sp"),
        P("sp", "tp"),
        P("tp"),
        P("tp", None),
        P(),
        P("sp", "tp"),
        P("sp", "tp"),
        P("tp", "sp"),
    )
    return jax.shard_map(
        local, mesh=mesh, in_specs=placed, out_specs=P("sp", "tp"), check_vma=False
    )
```

```python
import jax
import jax.numpy as jnp
from jax import lax
from jax.experimental import pallas as pl
from jax.experimental.pallas import tpu as pltpu
from jax.sharding import PartitionSpec as P

LOWEST_LOG = -1e30
EPSILON = 1e-06


def shift_pairs(length, step):
    return [(source, source + step) for source in range(length - step)]


def entering_state(state, top, total):
    length, index = lax.axis_size("sp"), lax.axis_index("sp")
    heads, key_width, value_width = state.shape

    def pack(s, t, f):
        tail = jnp.zeros((heads, 8, value_width), jnp.float32)
        tail = tail.at[:, 0, :].set(t[:, None]).at[:, 1, :].set(f[:, None])
        return jnp.concatenate([s, tail], axis=1)

    def unpack(p, valid):
        s = p[:, :key_width, :]
        t = jnp.where(valid, p[:, key_width, 0], LOWEST_LOG)
        f = jnp.where(valid, p[:, key_width + 1, 0], 0.0)
        return jnp.where(valid, s, 0.0), t, f

    moved = lax.ppermute(pack(state, top, total), "sp", shift_pairs(length, 1))
    s, t, f = unpack(moved, index >= 1)
    step = 1
    while step < length - 1:
        moved = lax.ppermute(pack(s, t, f), "sp", shift_pairs(length, step))
        s0, t0, f0 = unpack(moved, index >= step)
        from_top = t0 + f
        new_top = jnp.maximum(from_top, t)
        s = (
            jnp.exp(from_top - new_top)[:, None, None] * s0
            + jnp.exp(t - new_top)[:, None, None] * s
        )
        t, f = new_top, f0 + f
        step *= 2
    return s, t


def cell_kernel(q_ref, k_ref, v_ref, a_ref, m_ref, c_ref, state_ref, open_ref, gain_ref, o_ref, *, scale):
    block = q_ref.shape[0]
    length = k_ref.shape[0]
    q = q_ref[...]
    first = pl.program_id(1) * block
    scores = lax.dot_general(
        q, k_ref[...], (((1,), (1,)), ((), ())), preferred_element_type=jnp.float32
    )
    rows = first + lax.broadcasted_iota(jnp.int32, (block, length), 0)
    cols = lax.broadcasted_iota(jnp.int32, (block, length), 1)
    weight = jnp.where(cols <= rows, jnp.exp(jnp.minimum(a_ref[0] - m_ref[0], 0.0)), 0.0)
    numer = jnp.dot(
        (scores * weight).astype(jnp.bfloat16), v_ref[...], preferred_element_type=jnp.float32
    )
    before = jnp.dot(q, state_ref[0].astype(jnp.bfloat16), preferred_element_type=jnp.float32)
    memory = (numer + c_ref[0] * before) * scale
    normal = memory * lax.rsqrt(jnp.mean(memory * memory, axis=-1, keepdims=True) + EPSILON)
    gate_open = jax.nn.sigmoid(open_ref[...].astype(jnp.float32))
    o_ref[...] = (normal * gain_ref[...].astype(jnp.float32) * gate_open).astype(o_ref.dtype)


def cell(queries, keys, values, a_log, m_col, c_col, state, open_logits, gain):
    heads, length = a_log.shape
    dk, dv = queries.shape[1] // heads, values.shape[1] // heads
    block = min(length, 256)
    return pl.pallas_call(
        lambda *refs: cell_kernel(*refs, scale=dk ** (-0.5)),
        grid=(heads, length // block),
        in_specs=[
            pl.BlockSpec((block, dk), lambda h, i: (i, h)),
            pl.BlockSpec((length, dk), lambda h, i: (0, h)),
            pl.BlockSpec((length, dv), lambda h, i: (0, h)),
            pl.BlockSpec((1, 1, length), lambda h, i: (h, 0, 0)),
            pl.BlockSpec((1, block, 1), lambda h, i: (h, i, 0)),
            pl.BlockSpec((1, block, 1), lambda h, i: (h, i, 0)),
            pl.BlockSpec((1, dk, dv), lambda h, i: (h, 0, 0)),
            pl.BlockSpec((block, dv), lambda h, i: (i, h)),
            pl.BlockSpec((1, dv), lambda h, i: (0, h)),
        ],
        out_specs=pl.BlockSpec((block, dv), lambda h, i: (i, h)),
        out_shape=jax.ShapeDtypeStruct((length, heads * dv), jnp.bfloat16),
        cost_estimate=pl.CostEstimate(
            flops=8 * heads * length * length * dv, bytes_accessed=6 * length * heads * dv, transcendentals=0
        ),
        name="cell",
    )(queries, keys, values, a_log[:, None, :], m_col[:, :, None], c_col[:, :, None], state, open_logits, gain)


def partner_pairs(count):
    return [(i, i ^ 1) for i in range(count)]


def ring_pairs(count, step):
    return [(i, (i + 2 * step) % count) for i in range(count)]


def product_scattered(rows, weight):
    count, index = lax.axis_size("tp"), lax.axis_index("tp")
    chips, core, chip = count // 2, index % 2, index // 2
    width = weight.shape[1] // count

    def product(block):
        columns = lax.dynamic_slice_in_dim(weight, block * width, width, 1)
        return jnp.dot(rows, columns, preferred_element_type=jnp.float32)

    def chip_sum(to):
        given = product(2 * to + 1 - core).astype(jnp.bfloat16)
        got = lax.ppermute(given, "tp", partner_pairs(count))
        return product(2 * to + core) + got.astype(jnp.float32)

    moved = []
    for step in range(1, chips):
        sent = chip_sum((chip + step) % chips).astype(jnp.bfloat16)
        moved.append(lax.ppermute(sent, "tp", ring_pairs(count, step)))
    total = chip_sum(chip)
    for part in moved:
        total = total + part.astype(jnp.float32)
    return total


def columns_gathered(block):
    count, index = lax.axis_size("tp"), lax.axis_index("tp")
    chips, core, chip = count // 2, index % 2, index // 2
    width = block.shape[1]
    whole = jnp.zeros((block.shape[0], count * width), block.dtype)
    held = [(chip, block)]
    for step in range(1, chips):
        moved = lax.ppermute(block, "tp", ring_pairs(count, step))
        held.append(((chip - step) % chips, moved))
    for place, piece in held:
        other = lax.ppermute(piece, "tp", partner_pairs(count))
        whole = lax.dynamic_update_slice(whole, piece, (0, (2 * place + core) * width))
        whole = lax.dynamic_update_slice(whole, other, (0, (2 * place + 1 - core) * width))
    return whole


def local(
    queries,
    cell_key_rows,
    cell_value_rows,
    output_gate_logits,
    input_gate_logits,
    forget_gate_logits,
    forget_extra_term,
    residual,
    head_norm_gain,
    cell_output_weight,
    feedforward_norm_gain,
    gate_projection_weight,
    up_projection_weight,
    down_projection_weight,
):
    whole_gate = lax.all_gather(gate_projection_weight, "sp", axis=0, tiled=True)
    whole_up = lax.all_gather(up_projection_weight, "sp", axis=0, tiled=True)
    length = queries.shape[0]
    heads = input_gate_logits.shape[0]
    dk, dv = queries.shape[1] // heads, cell_value_rows.shape[1] // heads
    log_forget = jax.nn.log_sigmoid(forget_gate_logits.astype(jnp.float32)) + forget_extra_term
    running = jnp.cumsum(log_forget, axis=-1)
    a_log = input_gate_logits.astype(jnp.float32) - running
    m_log = lax.cummax(a_log, axis=1)
    a_top, total = m_log[:, -1], running[:, -1]
    decay = jnp.exp(a_log - a_top[:, None])
    weighed = (
        cell_key_rows.reshape(length, heads, dk).astype(jnp.float32) * decay.T[:, :, None]
    ).astype(jnp.bfloat16)
    state = jnp.stack(
        [
            lax.dot_general(
                weighed[:, h],
                cell_value_rows[:, h * dv : (h + 1) * dv],
                (((0,), (0,)), ((), ())),
                preferred_element_type=jnp.float32,
            )
            for h in range(heads)
        ]
    )
    carried, carried_top = entering_state(state, a_top + total, total)
    m_all = jnp.maximum(m_log, carried_top[:, None])
    coefficient = jnp.exp(carried_top[:, None] - m_all)
    gated = cell(
        queries,
        cell_key_rows,
        cell_value_rows,
        a_log,
        m_all,
        coefficient,
        carried,
        output_gate_logits,
        head_norm_gain[None, :],
    )
    summed = product_scattered(gated, cell_output_weight)
    stream = (residual.astype(jnp.float32) + summed).astype(jnp.bfloat16)
    down_late, stream = lax.optimization_barrier((down_projection_weight, stream))
    whole_down = lax.all_gather(down_late, "sp", axis=1, tiled=True)
    wide = columns_gathered(stream).astype(jnp.float32)
    scale = lax.rsqrt(jnp.mean(wide * wide, axis=-1, keepdims=True) + EPSILON)
    normed = (wide * scale * feedforward_norm_gain.astype(jnp.float32)[None, :]).astype(jnp.bfloat16)
    gate_value = jnp.dot(normed, whole_gate, preferred_element_type=jnp.float32)
    lifted = jnp.dot(normed, whole_up, preferred_element_type=jnp.float32)
    hidden = (jax.nn.silu(gate_value) * lifted).astype(jnp.bfloat16)
    channel_total = product_scattered(hidden, whole_down)
    return (stream.astype(jnp.float32) + 0.5 * channel_total).astype(jnp.bfloat16)


def solution(mesh):
    placed = (
        P("sp", "tp"),
        P("sp", "tp"),
        P("sp", "tp"),
        P("sp", "tp"),
        P("tp", "sp"),
        P("tp", "sp"),
        P("tp", "sp"),
        P("sp", "tp"),
        P("tp"),
        P("tp", None),
        P(),
        P("sp", "tp"),
        P("sp", "tp"),
        P("tp", "sp"),
    )
    return jax.shard_map(
        local, mesh=mesh, in_specs=placed, out_specs=P("sp", "tp"), check_vma=False
    )
```
